512 devices in a mesh: ep: 32 (over z, x), tp: 16 (over y, core).
Axes of the slice: x: 4, y: 8, z: 8, core: 2. Of those that a mesh axis runs over, the one named last changes fastest.
Arguments:
- mixer_query: bfloat16 [8192, 2048], P('ep', 'tp'), may hold values from -6 to 6
- mixer_forget: bfloat16 [8192, 2048], P('ep', 'tp'), may hold values from -5.5 to 5.5
- mixer_value: bfloat16 [8192, 2048], P('ep', 'tp'), may hold values from -6 to 6
- mixer_gate: bfloat16 [8192, 2048], P('ep', 'tp'), may hold values from -6 to 6
- forget_floor: float32 [2048], P('tp'), may hold values from 0.88 to 1
- head_gain: float32 [128], replicated, may hold values from 0.1 to 1.9
- mixer_proj: bfloat16 [2048, 2048], P(None, 'tp'), may hold values from -0.125 to 0.125
- expert_tokens: bfloat16 [4096, 2048], P('ep'), may hold values from -6 to 6
- expert_gain: float32 [2048], replicated, may hold values from 0.1 to 1.9
- routes: int32 [4096, 2], P('ep'), may hold values from 0 to 31, as said below
- group_logits: float32 [4096, 4], P('ep'), may hold values from -6 to 6
- choice_logits: float32 [4096, 2], P('ep'), may hold values from -6 to 6
- w_gate: bfloat16 [32, 2048, 2048], P('ep', None, 'tp'), may hold values from -0.125 to 0.125
- w_up: bfloat16 [32, 2048, 2048], P('ep', None, 'tp'), may hold values from -0.125 to 0.125
- w_down: bfloat16 [32, 2048, 2048], P('ep', None, 'tp'), may hold values from -0.125 to 0.125
Outputs:
- mixer_out: bfloat16 [8192, 2048], P('ep', 'tp')
- expert_out: bfloat16 [4096, 2048], P('ep', 'tp')
The draws below stay inside these ranges and needn't reach their ends.
Inputs may be any that keep to these rules, and one draw needn't show every extreme that they name: `routes`: in each aligned block of 128 rows (the rows of one index of ep) no expert is named by more than 16 rows, and some expert reaches that bound in every block; the 2 experts of a row differ and lie in the same group.
All inputs are finite; a program needn't handle non-finite values.
Results may differ from the reference program's by a relative error of at most 0.01.
Values may be sent and summed in bfloat16 or wider, within the bound.
A program may use at most 64 MiB of HBM per device.

```python
import math
import jax
import jax.numpy as jnp
from jax import lax

D = 2048
HEADS = 16
KEYDIM = 128
VDIM = 128
FF = 2048
GROUPS = 4
TOPK = 2
BLOCK = 64
TOKA_DEV = 256
TOKB_DEV = 128
EXPERTS = 32
EXP_GROUP = 8
CAP = 16
TOKENS_A = 8192
TOKENS_B = 4096
N_EP = 32


def draw_mixer_forget(key, part):
    noise_key = jax.random.fold_in(key, 11)
    shift_key = jax.random.fold_in(key, 12)
    noise = jnp.clip(jax.random.normal(noise_key, (TOKENS_A, HEADS * KEYDIM), jnp.float32), -4.0, 4.0)
    shifts = jax.random.uniform(shift_key, (TOKENS_A // TOKA_DEV, 1, 1), jnp.float32, -1.5, 1.5)
    shaped = noise.reshape(TOKENS_A // TOKA_DEV, TOKA_DEV, HEADS * KEYDIM) + shifts
    return shaped.reshape(TOKENS_A, HEADS * KEYDIM).astype(jnp.bfloat16)


def draw_forget_floor(key, part):
    pick_key = jax.random.fold_in(key, 21)
    slow_key = jax.random.fold_in(key, 22)
    fast_key = jax.random.fold_in(key, 23)
    slow_share = 0.5
    slow_heads = jax.random.uniform(pick_key, (HEADS, 1), jnp.float32) < slow_share
    slow_gap = jax.random.uniform(slow_key, (HEADS, KEYDIM), jnp.float32, 0.3, 2.0) / TOKENS_A
    fast_gap = jnp.exp(jax.random.uniform(fast_key, (HEADS, KEYDIM), jnp.float32, math.log(0.03), math.log(0.12)))
    gap_rows = jnp.where(slow_heads, slow_gap, fast_gap)
    return (1.0 - gap_rows).reshape(HEADS * KEYDIM).astype(jnp.float32)


def route_block(block_key):
    group_size = EXPERTS // GROUPS
    quota = TOKB_DEV // EXPERTS
    expert_ids = jnp.arange(EXPERTS, dtype=jnp.int32)
    counts = jnp.full((EXPERTS,), quota, jnp.int32)
    counts = counts + quota * ((expert_ids == 0) | (expert_ids == group_size - 1)).astype(jnp.int32)
    counts = counts - quota * ((expert_ids == group_size) | (expert_ids == group_size + 1)).astype(jnp.int32)
    canonical = jnp.repeat(expert_ids, counts, total_repeat_length=TOKB_DEV)
    order = jax.random.permutation(jax.random.fold_in(block_key, 1), TOKB_DEV)
    first = canonical[order]
    second = first // group_size * group_size + (first % group_size + 1) % group_size
    group_map = jax.random.permutation(jax.random.fold_in(block_key, 2), GROUPS).astype(jnp.int32)
    rotation = jax.random.randint(jax.random.fold_in(block_key, 3), (GROUPS,), 0, group_size).astype(jnp.int32)

    def relabel(ids):
        grp = ids // group_size
        return (group_map[grp] * group_size + (ids % group_size + rotation[grp]) % group_size).astype(jnp.int32)
    first = relabel(first)
    second = relabel(second)
    flip = jax.random.randint(jax.random.fold_in(block_key, 4), (TOKB_DEV,), 0, 2).astype(jnp.int32)
    left = flip * second + (1 - flip) * first
    right = flip * first + (1 - flip) * second
    return jnp.stack([left, right], axis=-1).astype(jnp.int32)


def draw_routes(key, part):
    base_key = jax.random.fold_in(key, 31)
    block_keys = jax.vmap(lambda index: jax.random.fold_in(base_key, index))(jnp.arange(N_EP))
    return jax.vmap(route_block)(block_keys).reshape(TOKENS_B, TOPK).astype(jnp.int32)


def steps_of(key, extent, cuts, least, largest):
    gain, own = 1.0, jax.random.fold_in(key, 6)
    for position, blocks in cuts:
        steps = jnp.exp(jax.random.uniform(jax.random.fold_in(own, position), (blocks,), jnp.float32, least / len(cuts), largest / len(cuts)))
        gain = gain * jnp.repeat(steps, extent[position] // blocks).reshape([-1 if axis == position else 1 for axis in range(len(extent))])
    return gain


def bell_draw(rng, shape, scale, bound, cuts=(), kind=jnp.bfloat16):
    loudness = steps_of(rng, shape, cuts, -0.22, 0.18) if cuts else 1.0
    values = jax.random.normal(rng, shape, jnp.float32) * scale * loudness
    return jnp.minimum(jnp.maximum(values, -bound), bound).astype(kind)


def setup_inputs(seed: int = 0) -> dict:
    key_of = jax.random.split(jax.random.key(seed), 16)
    return {
        "mixer_query": bell_draw(key_of[0], (TOKENS_A, HEADS * KEYDIM), 1.0, 6.0, ((0, 32), (1, 16))),
        "mixer_forget": draw_mixer_forget(jax.random.fold_in(key_of[15], 71), 0),
        "mixer_value": bell_draw(key_of[2], (TOKENS_A, HEADS * VDIM), 1.0, 6.0, ((0, 32), (1, 16))),
        "mixer_gate": bell_draw(key_of[3], (TOKENS_A, HEADS * VDIM), 1.0, 6.0, ((0, 32), (1, 16))),
        "forget_floor": draw_forget_floor(jax.random.fold_in(key_of[15], 71), 0),
        "head_gain": jnp.clip(1.0 + 0.18 * jax.random.normal(key_of[5], (VDIM,), jnp.float32), 0.1, 1.9),
        "mixer_proj": bell_draw(key_of[6], (HEADS * VDIM, D), (HEADS * VDIM) ** -0.5, 0.125, ((1, 16),)),
        "expert_tokens": bell_draw(key_of[7], (TOKENS_B, D), 1.0, 6.0, ((0, 32),)),
        "expert_gain": jnp.clip(1.0 + 0.18 * jax.random.normal(key_of[8], (D,), jnp.float32), 0.1, 1.9),
        "routes": draw_routes(jax.random.fold_in(key_of[15], 71), 0),
        "group_logits": bell_draw(key_of[10], (TOKENS_B, GROUPS), 1.0, 6.0, ((0, 32),), jnp.float32),
        "choice_logits": bell_draw(key_of[11], (TOKENS_B, TOPK), 1.0, 6.0, ((0, 32),), jnp.float32),
        "w_gate": bell_draw(key_of[12], (EXPERTS, D, FF), D ** -0.5, 0.125, ((0, 32), (2, 16))),
        "w_up": bell_draw(key_of[13], (EXPERTS, D, FF), D ** -0.5, 0.125, ((0, 32), (2, 16))),
        "w_down": bell_draw(key_of[14], (EXPERTS, FF, D), FF ** -0.5, 0.125, ((0, 32), (2, 16))),
    }


norm_eps = 1e-06
highest_precision = lax.Precision.HIGHEST

def rms_scale(features, gain_vec):
    return features * lax.rsqrt(lax.optimization_barrier(jnp.mean(features * features, axis=-1, keepdims=True)) + norm_eps) * gain_vec

def block_terms(query_block, input_block, log_blk, value_block, carried_state):
    cumulative_log = jnp.cumsum(log_blk, axis=0)
    between_block_term = jnp.einsum('zug,ugr->zur', query_block * jnp.exp(cumulative_log), carried_state, precision=highest_precision)
    causal = jnp.tril(jnp.ones((query_block.shape[0], query_block.shape[0]), dtype=bool))[:, :, None, None]
    differ = cumulative_log[:, None] - cumulative_log[None, :]
    decays = jnp.exp(jnp.where(causal, differ, -jnp.inf))
    scores = lax.optimization_barrier(jnp.sum(query_block[:, None] * input_block[None, :] * decays, axis=-1))
    result = between_block_term + jnp.einsum('tsh,shv->thv', scores, value_block, precision=highest_precision)
    ending_log_decay = cumulative_log[-1]
    updated_state = jnp.exp(ending_log_decay)[..., None] * carried_state + jnp.einsum('twa,twr->war', input_block * jnp.exp(ending_log_decay[None] - cumulative_log), value_block, precision=highest_precision)
    return (updated_state, result, cumulative_log)

def mixer_part(mixer_query, mixer_forget, mixer_value, mixer_gate, forget_floor, head_gain, mixer_proj):
    length = mixer_query.shape[0]
    blocks = length // BLOCK

    def split_blocks(source_array, last_width):
        return source_array.reshape(blocks, BLOCK, HEADS, last_width)
    queries = jax.nn.silu(mixer_query.astype(jnp.float32))
    input_rates = (1.0 - forget_floor) * jax.nn.sigmoid(-mixer_forget.astype(jnp.float32))
    log_forget = jnp.log1p(-input_rates)
    value_rows = mixer_value.astype(jnp.float32)

    def advance(carried_state, block_inputs):
        query_block, input_block, value_block, log_blk = block_inputs
        updated_state, result, cumulative_log = block_terms(query_block, input_block, log_blk, value_block, carried_state)
        return (updated_state, result)
    initial = jnp.zeros((HEADS, KEYDIM, VDIM), jnp.float32)
    _, output_rows = lax.scan(advance, initial, (split_blocks(queries, KEYDIM), split_blocks(input_rates, KEYDIM), split_blocks(value_rows, VDIM), split_blocks(log_forget, KEYDIM)))
    output_rows = output_rows.reshape(length, HEADS, VDIM)
    gate_act = jax.nn.silu(mixer_gate.astype(jnp.float32)).reshape(length, HEADS, VDIM)
    gated_out = rms_scale(output_rows, head_gain) * gate_act
    mixed_heads = gated_out.reshape(length, HEADS * VDIM).astype(jnp.bfloat16)
    return jnp.dot(mixed_heads, mixer_proj, preferred_element_type=jnp.float32).astype(jnp.bfloat16)

def gate_weights(routes, group_logits, choice_logits, group_size):
    group_exp = jnp.exp(group_logits)
    group_prob = group_exp / lax.optimization_barrier(jnp.sum(group_exp, axis=-1, keepdims=True))
    groups_of = routes // group_size
    member = (groups_of[..., None] == jnp.arange(GROUPS, dtype=jnp.int32)).astype(jnp.float32)
    picked_prob = lax.optimization_barrier(jnp.sum(member * group_prob[:, None, :], axis=-1))
    choice_exp = jnp.exp(choice_logits)
    together = (groups_of[:, :, None] == groups_of[:, None, :]).astype(jnp.float32)
    within = lax.optimization_barrier(jnp.sum(together * choice_exp[:, None, :], axis=-1))
    return picked_prob * choice_exp / within

def rank_slots(flat_routes, per_block, expert_count):
    onehot = (flat_routes[:, None] == jnp.arange(expert_count, dtype=jnp.int32)).astype(jnp.int32)
    blocked = onehot.reshape(-1, per_block, expert_count)
    earlier = (jnp.cumsum(blocked, axis=1) - blocked).astype(jnp.int32)
    return lax.optimization_barrier(jnp.sum(earlier * blocked, axis=-1)).astype(jnp.int32).reshape(-1)

def expert_part(expert_tokens, expert_gain, routes, group_logits, choice_logits, w_gate, w_up, w_down):
    count_rows = expert_tokens.shape[0]
    normed = rms_scale(expert_tokens.astype(jnp.float32), expert_gain).astype(jnp.bfloat16)
    weights = gate_weights(routes, group_logits, choice_logits, EXP_GROUP)
    flat_routes = routes.reshape(-1)
    per_block = TOKB_DEV * TOPK
    ranks = rank_slots(flat_routes, per_block, EXPERTS)
    block_ids = (jnp.arange(flat_routes.shape[0], dtype=jnp.int32) // per_block).astype(jnp.int32)
    slot_of = (flat_routes * (N_EP * CAP) + block_ids * CAP + ranks).astype(jnp.int32)
    token_ids = (jnp.arange(flat_routes.shape[0], dtype=jnp.int32) // TOPK).astype(jnp.int32)
    token_of = jnp.full((EXPERTS * N_EP * CAP,), count_rows, jnp.int32).at[slot_of].set(token_ids)
    padded = jnp.concatenate([normed, jnp.zeros((1, D), jnp.bfloat16)], axis=0)

    def run_expert(operands):
        gate_mat, up_mat, down_mat, index_rows = operands
        chosen = padded[index_rows]
        gate_pre = jnp.dot(chosen, gate_mat, preferred_element_type=jnp.float32)
        up_pre = jnp.dot(chosen, up_mat, preferred_element_type=jnp.float32)
        hidden = (jax.nn.silu(gate_pre) * up_pre).astype(jnp.bfloat16)
        return jnp.dot(hidden, down_mat, preferred_element_type=jnp.float32).astype(jnp.bfloat16)
    output_rows = lax.map(run_expert, (w_gate, w_up, w_down, token_of.reshape(EXPERTS, N_EP * CAP)))
    picked = output_rows.reshape(-1, D)[slot_of].astype(jnp.float32) * weights.reshape(-1)[:, None]
    return lax.optimization_barrier(jnp.sum(picked.reshape(count_rows, TOPK, D), axis=1)).astype(jnp.bfloat16)

def reference(mixer_query, mixer_forget, mixer_value, mixer_gate, forget_floor, head_gain, mixer_proj, expert_tokens, expert_gain, routes, group_logits, choice_logits, w_gate, w_up, w_down):
    mixer_out = mixer_part(mixer_query, mixer_forget, mixer_value, mixer_gate, forget_floor, head_gain, mixer_proj)
    expert_out = expert_part(expert_tokens, expert_gain, routes, group_logits, choice_logits, w_gate, w_up, w_down)
    return (mixer_out, expert_out)
```

```python
import jax
import jax.numpy as jnp
from jax import lax
from jax.experimental import pallas as pl
from jax.experimental.pallas import tpu as pltpu
from jax.sharding import Mesh
from jax.sharding import PartitionSpec as P

NZ, NX, NY, NC = 8, 4, 8, 2
EXPERTS = NZ * NX
TP = NY * NC
GROUPS = 4
EXP_GROUP = EXPERTS // GROUPS
CAP = 16
SLOTS = EXPERTS * CAP
LANES = 128
TOKENS_A = 256
TOKENS_B = 128
WIDTH = 2048
CHUNK = 128
MSG = 48
SLICE = LANES // NX
MESH = pl.DeviceIdType.MESH
norm_eps = 1e-06

f32, bf16, i32 = jnp.float32, jnp.bfloat16, jnp.int32


def remote(src, dst, send_sem, recv_sem, **where):
    return pltpu.make_async_remote_copy(
        src_ref=src,
        dst_ref=dst,
        send_sem=send_sem,
        recv_sem=recv_sem,
        device_id=where,
        device_id_type=MESH,
    )


def drain(view, sem):
    pltpu.make_async_copy(view, view, sem).wait()


def sigmoid(v):
    return jax.nn.sigmoid(v)


def halves(v):
    high = v.astype(bf16)
    return high, (v - high.astype(f32)).astype(bf16)


def nn(a, b):
    return lax.dot_general(a, b, (((1,), (0,)), ((), ())), preferred_element_type=f32)


def nt(a, b):
    return lax.dot_general(a, b, (((1,), (1,)), ((), ())), preferred_element_type=f32)


class Ring:
    def __init__(self, buf, sems, y, c):
        self.buf, self.y, self.c = buf, y, c
        self.send, self.from_left, self.from_right, self.pair_send, self.pair_recv = sems
        self.chunks = buf.shape[1] // CHUNK
        self.right, self.left = lax.rem(y + 1, NY), lax.rem(y + NY - 1, NY)

    def at(self, chip, q):
        return self.buf.at[chip * NC + self.c, pl.ds(q * CHUNK, CHUNK)]

    def reach(self, q):
        return (4, 3) if q % 2 == 0 else (3, 4)

    def go_right(self, chip, hop, q):
        v = self.at(chip, q)
        return remote(v, v, self.send.at[0], self.from_left.at[hop, q], y=self.right)

    def go_left(self, chip, hop, q):
        v = self.at(chip, q)
        return remote(v, v, self.send.at[0], self.from_right.at[hop, q], y=self.left)

    def pair(self, chip, q):
        v = self.at(chip, q)
        return remote(v, v, self.pair_send.at[0], self.pair_recv.at[q], c=1 - self.c)

    def start(self, q):
        self.go_right(self.y, 0, q).start()
        self.go_left(self.y, 0, q).start()
        self.pair(self.y, q).start()

    def step(self, hop, q):
        to_right, to_left = self.reach(q)
        if hop <= to_right:
            chip = lax.rem(self.y + NY - hop, NY)
            self.go_right(chip, hop - 1, q).wait_recv()
            if hop < to_right:
                self.go_right(chip, hop, q).start()
            self.pair(chip, q).start()
        if hop <= to_left:
            chip = lax.rem(self.y + hop, NY)
            self.go_left(chip, hop - 1, q).wait_recv()
            if hop < to_left:
                self.go_left(chip, hop, q).start()
            self.pair(chip, q).start()

    def finish(self, q):
        drain(self.buf.at[pl.ds(0, NY), pl.ds(q * CHUNK, CHUNK)], self.pair_recv.at[q])

    def rows(self, q, count=1):
        return jnp.concatenate(
            [self.buf[k, q * CHUNK : (q + count) * CHUNK] for k in range(TP)], axis=1
        )

    def sent(self):
        drain(self.buf.at[pl.ds(0, NY - 1)], self.send.at[0])
        drain(self.buf.at[pl.ds(0, NY)], self.pair_send.at[0])


def ring_sems(chunks):
    dma = pltpu.SemaphoreType.DMA
    return [dma((1,)), dma((4, chunks)), dma((4, chunks)), dma((1,)), dma((chunks,))]


def kernel(
    query_hbm, forget_hbm, value_hbm, gate_hbm, floor_hbm, head_gain_hbm, proj_hbm,
    tokens_hbm, gain_hbm, routes_hbm, group_hbm, choice_hbm, wg_hbm, wu_hbm, wd_hbm,
    mixer_ref, expert_ref,
    query, forget, value, gate, floor, head_gain, proj, tokens, gain, routes, group,
    choice, wgu, wd, outgoing, back, values, combine_hi, combine_lo, xbuf, hbuf, mbuf,
    x1_send, x1_recv, z2_send, z2_recv, x3_send, incoming,
    load_sem, disp_send, disp_recv, back_sem, mix_sem, *ring_scratch,
):
    z, x = lax.axis_index("z"), lax.axis_index("x")
    y, c = lax.axis_index("y"), lax.axis_index("c")
    me, piece = z * NX + x, y * NC + c

    offsets = [(dz, dx) for dz in range(NZ) for dx in range(NX) if (dz, dx) != (0, 0)]
    far = lambda o: min(o[0], NZ - o[0]) + min(o[1], NX - o[1])
    offsets.sort(key=far, reverse=True)

    def peer(dz, dx):
        return lax.rem(z + dz, NZ), lax.rem(x + dx, NX)

    barrier = pltpu.get_barrier_semaphore()
    for dz, dx in offsets:
        tz, tx = peer(dz, dx)
        pl.semaphore_signal(barrier, inc=1, device_id={"z": tz, "x": tx}, device_id_type=MESH)
    for there in ({"y": lax.rem(y + 1, NY)}, {"y": lax.rem(y + NY - 1, NY)}, {"c": 1 - c}):
        pl.semaphore_signal(barrier, inc=1, device_id=there, device_id_type=MESH)

    loads = [
        pltpu.make_async_copy(src, dst, load_sem.at[k])
        for k, (src, dst) in enumerate(
            [
                (tokens_hbm, tokens), (gain_hbm, gain), (routes_hbm, routes),
                (group_hbm, group), (choice_hbm, choice), (query_hbm, query),
                (forget_hbm, forget), (value_hbm, value), (gate_hbm, gate),
                (floor_hbm, floor), (head_gain_hbm, head_gain),
                (wg_hbm, wgu.at[:, pl.ds(0, LANES)]), (wu_hbm, wgu.at[:, pl.ds(LANES, LANES)]),
                (wd_hbm, wd), (proj_hbm, proj),
            ]
        )
    ]
    for load in loads:
        load.start()

    xring = Ring(xbuf, ring_scratch[0:5], y, c)
    hring = Ring(hbuf, ring_scratch[5:10], y, c)
    mring = Ring(mbuf, ring_scratch[10:15], y, c)

    for load in loads[0:5]:
        load.wait()
    route_rows = [routes[j : j + 1, :] for j in range(2)]
    expert_ids = lax.broadcasted_iota(i32, (EXPERTS, TOKENS_B), 0)
    onehots = [(expert_ids == r).astype(f32) for r in route_rows]
    earlier = (
        lax.broadcasted_iota(i32, (TOKENS_B, TOKENS_B), 0)
        < lax.broadcasted_iota(i32, (TOKENS_B, TOKENS_B), 1)
    ).astype(bf16)
    firsts = nn(onehots[0].astype(bf16), earlier)
    seconds = nn(onehots[1].astype(bf16), earlier) + jnp.sum(onehots[0], axis=1, keepdims=True)
    ranks = [
        jnp.sum(h * n, axis=0, keepdims=True) for h, n in zip(onehots, (firsts, seconds))
    ]
    slot_ids = lax.broadcasted_iota(i32, (SLOTS, TOKENS_B), 0)
    members = [
        slot_ids == r * CAP + n.astype(i32) for r, n in zip(route_rows, ranks)
    ]
    picks = jnp.logical_or(members[0], members[1]).astype(f32).astype(bf16)
    token_rows = tokens[...].astype(f32)
    scale = lax.rsqrt(jnp.mean(token_rows * token_rows, axis=1, keepdims=True) + norm_eps)
    columns = pl.ds(pl.multiple_of(piece * LANES, LANES), LANES)
    normed = (tokens[:, columns].astype(f32) * scale * gain[:, columns]).astype(bf16)
    outgoing[...] = nn(picks, normed).astype(bf16)

    pl.semaphore_wait(barrier, len(offsets) + 3)
    for dz, dx in offsets:
        tz, tx = peer(dz, dx)
        there = tz * NX + tx
        remote(
            outgoing.at[pl.ds(there * CAP, CAP)],
            xbuf.at[piece, pl.ds(me * CAP, CAP)],
            disp_send.at[0],
            disp_recv.at[z // 2],
            z=tz,
            x=tx,
        ).start()
    mine = pl.ds(pl.multiple_of(me * CAP, CAP), CAP)
    xbuf[piece, mine] = outgoing[mine, :]

    for load in loads[5:11]:
        load.wait()
    query_pre = query[...].astype(f32)
    queries = query_pre * sigmoid(query_pre)
    rates = (1.0 - floor[...]) * sigmoid(-forget[...].astype(f32))
    log_forget = jnp.log1p(-rates)
    row_ids = lax.broadcasted_iota(i32, (TOKENS_A, TOKENS_A), 0)
    col_ids = lax.broadcasted_iota(i32, (TOKENS_A, TOKENS_A), 1)
    causal = col_ids <= row_ids
    triangle = causal.astype(f32).astype(bf16)
    log_hi = log_forget.astype(bf16)
    log_mid, log_lo = halves(log_forget - log_hi.astype(f32))
    total = nn(triangle, log_hi) + (nn(triangle, log_mid) + nn(triangle, log_lo))
    last = total[TOKENS_A - 1 : TOKENS_A, :]
    keys_end = rates * jnp.exp(last - total)
    value_t = jnp.transpose(value[...].astype(f32)).astype(bf16)
    end_hi, end_lo = halves(keys_end)
    state = nn(value_t, end_hi) + nn(value_t, end_lo)
    last_hi = last.astype(bf16)
    last_mid, last_lo = halves(last - last_hi.astype(f32))

    def pack(ref, part, logs):
        hi = logs.astype(bf16)
        mid, lo = halves(logs - hi.astype(f32))
        rows = jnp.concatenate(
            [part, hi.astype(f32), mid.astype(f32), lo.astype(f32),
             jnp.zeros((MSG - SLICE - 3, LANES), f32)], axis=0)
        ref[...] = rows.astype(bf16)

    def unpack(msg):
        rows = msg.astype(f32)
        logs = rows[SLICE : SLICE + 1] + rows[SLICE + 1 : SLICE + 2] + rows[SLICE + 2 : SLICE + 3]
        return rows[0:SLICE], logs

    for k in range(NX):
        pack(x1_send.at[k], state[k * SLICE : (k + 1) * SLICE], last)
    for d in range(1, NX):
        tx = lax.rem(x + d, NX)
        remote(x1_send.at[tx], x1_recv.at[x], mix_sem.at[0], mix_sem.at[1], x=tx).start()
    x1_recv[x] = x1_send[x]

    queries_hi, queries_lo = halves(queries * jnp.exp(total))
    keys_hi, keys_lo = halves(rates * jnp.exp(-total))
    scores = nt(queries_hi, keys_hi) + (nt(queries_hi, keys_lo) + nt(queries_lo, keys_hi))
    scores_hi, scores_lo = halves(jnp.where(causal, scores, 0.0))
    inner = nn(scores_hi, value[...]) + nn(scores_lo, value[...])
    gate_pre = gate[...].astype(f32)
    gate_act = gate_pre * sigmoid(gate_pre) * head_gain[...]

    drain(x1_recv.at[pl.ds(0, NX - 1)], mix_sem.at[1])
    parts = [unpack(x1_recv[k]) for k in range(NX)]
    before = [(jnp.zeros((SLICE, LANES), f32), jnp.zeros((1, LANES), f32))]
    for part, logs in parts:
        so_far, log_so_far = before[-1]
        before.append((jnp.exp(logs) * so_far + part, log_so_far + logs))
    pack(z2_send, *before[NX])
    for d in range(1, NZ):
        tz = lax.rem(z + d, NZ)
        remote(z2_send, z2_recv.at[z], mix_sem.at[2], mix_sem.at[3], z=tz).start()
    z2_recv[z] = z2_send[...]

    group_exp = jnp.exp(group[...])
    group_prob = group_exp / jnp.sum(group_exp, axis=0, keepdims=True)
    groups_of = [r // EXP_GROUP for r in route_rows]
    group_ids = lax.broadcasted_iota(i32, (GROUPS, TOKENS_B), 0)
    picked = [
        jnp.sum(jnp.where(group_ids == g, group_prob, 0.0), axis=0, keepdims=True)
        for g in groups_of
    ]
    choice_exp = jnp.exp(choice[...])
    exps = [choice_exp[j : j + 1] for j in range(2)]
    together = (groups_of[0] == groups_of[1]).astype(f32)
    weights = [
        picked[0] * exps[0] / (exps[0] + together * exps[1]),
        picked[1] * exps[1] / (exps[1] + together * exps[0]),
    ]
    spread = jnp.where(members[0], weights[0], 0.0) + jnp.where(members[1], weights[1], 0.0)
    combine = jnp.transpose(spread)
    high, low = halves(combine)
    combine_hi[...] = high
    combine_lo[...] = low

    chunks = SLOTS // CHUNK
    own = z // 2
    for q in range(chunks):
        rows = q * CHUNK

        @pl.when(own == q)
        def _():
            drain(outgoing.at[pl.ds(rows, CHUNK - CAP)], disp_recv.at[q])

        @pl.when(own != q)
        def _():
            drain(outgoing.at[pl.ds(rows, CHUNK)], disp_recv.at[q])

        xring.start(q)
    for q in range(chunks):
        xring.step(1, q)

    drain(z2_recv.at[pl.ds(0, NZ - 1)], mix_sem.at[3])
    prefix = jnp.zeros((SLICE, LANES), f32)
    for k in range(NZ):
        part, logs = unpack(z2_recv[k])
        prefix = jnp.where(k < z, jnp.exp(logs) * prefix + part, prefix)
    for k in range(NX):
        x3_send[k] = (jnp.exp(before[k][1]) * prefix + before[k][0]).astype(bf16)
    mine3 = pl.ds(pl.multiple_of(x * SLICE, SLICE), SLICE)
    for d in range(1, NX):
        tx = lax.rem(x + d, NX)
        remote(x3_send.at[tx], incoming.at[mine3], mix_sem.at[4], mix_sem.at[5], x=tx).start()
    incoming[mine3, :] = x3_send[x]

    for q in range(chunks):
        xring.step(2, q)

    drain(incoming.at[pl.ds(0, LANES - SLICE)], mix_sem.at[5])
    state_in = incoming[...]
    recurrent = inner + (nt(queries_hi, state_in) + nt(queries_lo, state_in))
    size = lax.rsqrt(jnp.mean(recurrent * recurrent, axis=1, keepdims=True) + norm_eps)
    mbuf[piece] = (recurrent * size * gate_act).astype(bf16)

    for q in range(chunks):
        xring.step(3, q)
    for q in range(TOKENS_A // CHUNK):
        mring.start(q)
    loads[11].wait()
    loads[12].wait()
    for q in range(chunks):
        xring.step(4, q)
        xring.finish(q)
        both = nn(xring.rows(q), wgu[...])
        pre = both[:, 0:LANES]
        hbuf[piece, q * CHUNK : (q + 1) * CHUNK] = (pre * sigmoid(pre) * both[:, LANES:]).astype(bf16)
        hring.start(q)
    for q in range(TOKENS_A // CHUNK):
        mring.step(1, q)
    for hop in (1, 2, 3):
        for q in range(chunks):
            hring.step(hop, q)
    for q in range(TOKENS_A // CHUNK):
        mring.step(2, q)
    loads[13].wait()
    for q in range(chunks):
        hring.step(4, q)
        hring.finish(q)
        values[q * CHUNK : (q + 1) * CHUNK] = nn(hring.rows(q), wd[...]).astype(bf16)
        for s in range(q * CHUNK // CAP, (q + 1) * CHUNK // CAP):
            sz, sx = s // NX, s % NX

            @pl.when(me != s)
            def _():
                remote(
                    values.at[pl.ds(s * CAP, CAP)],
                    back.at[pl.ds(me * CAP, CAP)],
                    back_sem.at[0],
                    back_sem.at[1],
                    z=sz,
                    x=sx,
                ).start()

            @pl.when(me == s)
            def _():
                back[s * CAP : (s + 1) * CAP] = values[s * CAP : (s + 1) * CAP]

    for hop in (3, 4):
        for q in range(TOKENS_A // CHUNK):
            mring.step(hop, q)
    loads[14].wait()
    for q in range(TOKENS_A // CHUNK):
        mring.finish(q)
    mixer_ref[...] = nn(mring.rows(0, TOKENS_A // CHUNK), proj[...]).astype(bf16)

    drain(back.at[pl.ds(0, SLOTS - CAP)], back_sem.at[1])
    returned = back[...]
    expert_ref[...] = (nn(combine_hi[...], returned) + nn(combine_lo[...], returned)).astype(bf16)

    drain(outgoing.at[pl.ds(0, SLOTS - CAP)], disp_send.at[0])
    drain(values.at[pl.ds(0, SLOTS - CAP)], back_sem.at[0])
    drain(x1_recv.at[pl.ds(0, NX - 1)], mix_sem.at[0])
    drain(z2_recv.at[pl.ds(0, NZ - 1)], mix_sem.at[2])
    drain(x3_send.at[pl.ds(0, NX - 1)], mix_sem.at[4])
    for ring in (xring, hring, mring):
        ring.sent()


def per_device(
    mixer_query, mixer_forget, mixer_value, mixer_gate, forget_floor, head_gain, mixer_proj,
    expert_tokens, expert_gain, routes, group_logits, choice_logits, w_gate, w_up, w_down,
):
    vmem, dma = pltpu.VMEM, pltpu.SemaphoreType.DMA
    args = (
        mixer_query, mixer_forget, mixer_value, mixer_gate,
        forget_floor.reshape(1, -1), head_gain.reshape(1, -1), mixer_proj,
        expert_tokens, expert_gain.reshape(1, -1),
        routes.T, group_logits.T, choice_logits.T,
        w_gate[0], w_up[0], w_down[0],
    )
    chunks = SLOTS // CHUNK
    scratch = [vmem(a.shape, a.dtype) for a in args[0:12]]
    scratch += [
        vmem((WIDTH, 2 * LANES), bf16),
        vmem((WIDTH, LANES), bf16),
        vmem((SLOTS, LANES), bf16),
        vmem((SLOTS, LANES), bf16),
        vmem((SLOTS, LANES), bf16),
        vmem((TOKENS_B, SLOTS), bf16),
        vmem((TOKENS_B, SLOTS), bf16),
        vmem((TP, SLOTS, LANES), bf16),
        vmem((TP, SLOTS, LANES), bf16),
        vmem((TP, TOKENS_A, LANES), bf16),
        vmem((NX, MSG, LANES), bf16),
        vmem((NX, MSG, LANES), bf16),
        vmem((MSG, LANES), bf16),
        vmem((NZ, MSG, LANES), bf16),
        vmem((NX, SLICE, LANES), bf16),
        vmem((LANES, LANES), bf16),
        dma((len(args),)),
        dma((1,)),
        dma((chunks,)),
        dma((2,)),
        dma((6,)),
    ]
    scratch += ring_sems(chunks) + ring_sems(chunks) + ring_sems(TOKENS_A // CHUNK)
    return pl.pallas_call(
        kernel,
        out_shape=(
            jax.ShapeDtypeStruct((TOKENS_A, LANES), bf16),
            jax.ShapeDtypeStruct((TOKENS_B, LANES), bf16),
        ),
        in_specs=[pl.BlockSpec(memory_space=pltpu.HBM)] * len(args),
        out_specs=(pl.BlockSpec(memory_space=vmem), pl.BlockSpec(memory_space=vmem)),
        scratch_shapes=scratch,
        compiler_params=pltpu.CompilerParams(
            collective_id=0, has_side_effects=True, vmem_limit_bytes=40 << 20
        ),
        name="hybrid_layer",
    )(*args)


def solution(mesh):
    finer = Mesh(mesh.devices.reshape(NZ, NX, NY, NC), ("z", "x", "y", "c"))
    ep, tp = ("z", "x"), ("y", "c")
    placed = (
        P(ep, tp),
        P(ep, tp),
        P(ep, tp),
        P(ep, tp),
        P(tp),
        P(),
        P(None, tp),
        P(ep, None),
        P(),
        P(ep, None),
        P(ep, None),
        P(ep, None),
        P(ep, None, tp),
        P(ep, None, tp),
        P(ep, None, tp),
    )
    return jax.shard_map(
        per_device,
        mesh=finer,
        in_specs=placed,
        out_specs=(P(ep, tp), P(ep, tp)),
        check_vma=False,
    )
```
